32 devices in a mesh: sp: 8 (over z, y), tp: 4 (over x, core).
Axes of the slice: x: 2, y: 2, z: 4, core: 2. Of those that a mesh axis runs over, the one named last changes fastest.
Arguments:
- conv_outer: bfloat16 [6144, 2048], P('sp', 'tp'), may hold values from -6 to 6
- conv_inner: bfloat16 [6144, 2048], P('sp', 'tp'), may hold values from -6 to 6
- conv_input: bfloat16 [6144, 2048], P('sp', 'tp'), may hold values from -6 to 6
- conv_taps: float32 [3, 2048], P(None, 'tp'), may hold values from -3.5 to 3.5
- out_weight: bfloat16 [2048, 2048], P('tp'), may hold values from -0.125 to 0.125
- mix_gate: bfloat16 [6144, 2048], P(('sp', 'tp')), may hold values from -8 to 8
- residual: bfloat16 [6144, 2048], P(('sp', 'tp')), may hold values from -6 to 6
- mix_gain: float32 [2048], replicated, may hold values from 0.1 to 1.9
- expert_gain: float32 [2048], replicated, may hold values from 0.1 to 1.9
- expert_ids: int32 [6144, 2], P(('sp', 'tp')), may hold values from 0 to 7, all different within a row; in each aligned block of 192 rows (0 to 191, 192 to 383, ...) at most 96 rows name the same one
- group_share: float32 [6144], P(('sp', 'tp')), may hold values from 0.25 to 1
- pair_scores: float32 [6144, 2], P(('sp', 'tp')), may hold values from -8 to 8
- gate_experts: bfloat16 [8, 2048, 512], P('sp'), may hold values from -0.125 to 0.125
- up_experts: bfloat16 [8, 2048, 512], P('sp'), may hold values from -0.125 to 0.125
- down_experts: bfloat16 [8, 512, 2048], P('sp'), may hold values from -0.25 to 0.25
Outputs:
- layer_out: bfloat16 [6144, 2048], P(('sp', 'tp'))
The draws below stay inside these ranges and needn't reach their ends.
Inputs may be any that keep to these rules, and one draw needn't show every extreme that they name: `expert_ids`: within the rows of one device (aligned blocks of 192 rows), no expert is named by more than 96 rows, a bound that some block reaches; the 2 experts of a row differ.
All inputs are finite; a program needn't handle non-finite values.
Results may differ from the reference program's by a relative error of at most 0.0069.
Values may be sent and summed in bfloat16 or wider, within the bound.
A program may use at most 128 MiB of HBM per device.

```python
import math
import jax
import jax.numpy as jnp
import numpy as np
from jax import lax

D = 2048
CW = 2048
FF = 512
KSIZE = 3
TOP = 2
TOK_DEV = 192
EXPERTS = 8
CAP = 96
TOKENS = 6144


def block_scale(stream_key, dims, cuts, smallest, largest):
    loudness, own = 1.0, jax.random.fold_in(stream_key, 6)
    for axis_at, blocks in cuts:
        steps = jnp.exp(jax.random.uniform(jax.random.fold_in(own, axis_at), (blocks,), jnp.float32, smallest / len(cuts), largest / len(cuts)))
        loudness = loudness * jnp.repeat(steps, dims[axis_at] // blocks).reshape([-1 if axis == axis_at else 1 for axis in range(len(dims))])
    return loudness


def routed_block(own_key, own, number, rows, amount, top, limit, skew):
    order = jax.random.permutation(own_key, amount)
    packed, ordinary = load_shares(amount, rows * top, limit, skew, True), load_shares(amount, rows * top, limit, skew, False)
    places = jnp.arange(amount)

    def named(sizes, rotation):
        used = int((sizes > 0).sum())
        fixed = max(1, used // 4)
        moved = fixed + (places - fixed + rotation * (used - fixed)) % max(1, amount - fixed)
        return jnp.zeros((amount,), jnp.int32).at[order[jnp.where(places < fixed, places, moved)]].set(jnp.asarray(sizes, jnp.int32))

    sizes = jnp.where(number % 4 == 0, named(packed, number // 4), named(ordinary, number - number // 4 - 1))
    mixed = jax.random.permutation(jax.random.fold_in(own, 3), amount)
    donor, sink = mixed[0:amount // 2 * 2:2], mixed[1:amount // 2 * 2:2]
    margin = jnp.minimum(sizes[donor] - 1, limit - sizes[sink]) // 2
    margin = jnp.where((donor == order[0]) | (sink == order[0]) | (sizes[sink] == 0), 0, jnp.maximum(margin, 0))
    moved = jax.random.randint(jax.random.fold_in(own, 4), (amount // 2,), 0, 1 << 20) % (margin + 1)
    sizes = sizes.at[donor].add(-moved).at[sink].add(moved)
    members = jnp.searchsorted(jnp.cumsum(sizes), jnp.arange(rows * top), side="right").astype(jnp.int32)
    table = members.reshape(top, rows).T
    table = table[jax.random.permutation(jax.random.fold_in(own, 1), rows)]
    rotation = jax.random.randint(jax.random.fold_in(own, 2), (rows, 1), 0, top)
    return jnp.take_along_axis(table, (jnp.arange(top)[None, :] + rotation) % top, axis=1)


def load_shares(number_of, total, reach, slope, full):
    portions = [(1 << 20) // math.isqrt(standing ** slope) + 1 for standing in range(1, number_of + 1)]
    largest = reach if full else min(reach, max(-(-total // number_of), total * portions[0] // sum(portions)))
    least = 1 if total - largest >= number_of - 1 else 0
    given, spare = [largest] + [least] * (number_of - 1), total - largest - least * (number_of - 1)
    while spare > 0:
        candidates = [i for i in range(1, number_of) if given[i] < largest] or [i for i in range(1, number_of) if given[i] < reach]
        mass, budget = sum([portions[i] for i in candidates]), spare
        for i in candidates:
            extra = min(reach - given[i], max(1, budget * portions[i] // mass), spare)
            given[i] = given[i] + extra
            spare = spare - extra
    return np.array(given)


def bell_draw(rng, extent, spread, limit, pieces=(), kind=jnp.bfloat16):
    level = block_scale(rng, extent, pieces, -0.22, 0.18) if pieces else 1.0
    values = jax.random.normal(rng, extent, jnp.float32) * spread * level
    return jnp.minimum(jnp.maximum(values, -limit), limit).astype(kind)


def setup_inputs(seed: int = 0) -> dict:
    key_list = jax.random.split(jax.random.key(seed), 16)
    conv_outer = bell_draw(key_list[0], (TOKENS, CW), 1.0, 6.0, ((0, 8), (1, 4)))
    conv_inner = bell_draw(key_list[1], (TOKENS, CW), 1.0, 6.0, ((0, 8), (1, 4)))
    conv_input = bell_draw(key_list[2], (TOKENS, CW), 1.0, 6.0, ((0, 8), (1, 4)))
    conv_taps = bell_draw(key_list[3], (KSIZE, CW), KSIZE ** -0.5, 3.5, ((1, 4),), jnp.float32)
    out_weight = bell_draw(key_list[4], (CW, D), CW ** -0.5, 0.125, ((0, 4),))
    mix_gate = bell_draw(key_list[5], (TOKENS, D), 1.5, 8.0, ((0, 32),))
    residual = bell_draw(key_list[6], (TOKENS, D), 1.0, 6.0, ((0, 32),))
    mix_gain = jnp.clip(1.0 + 0.18 * jax.random.normal(key_list[7], (D,), jnp.float32), 0.1, 1.9)
    expert_gain = jnp.clip(1.0 + 0.18 * jax.random.normal(key_list[8], (D,), jnp.float32), 0.1, 1.9)
    expert_ids_keys = jax.random.split(jax.random.fold_in(key_list[9], 1), TOKENS // TOK_DEV)
    expert_ids_turns = jax.random.permutation(jax.random.fold_in(key_list[9], 3), TOKENS // TOK_DEV)
    expert_ids = jax.vmap(lambda own, number: routed_block(jax.random.fold_in(key_list[9], 2), own, number, TOK_DEV, EXPERTS, TOP, CAP, 1))(expert_ids_keys, expert_ids_turns).reshape((TOKENS, TOP))
    group_share = jnp.clip(0.25 + 0.75 * jax.random.uniform(key_list[10], (TOKENS,), jnp.float32) ** block_scale(key_list[10], (TOKENS,), ((0, 32),), -0.2, 0.2), 0.25, 1.0)
    pair_scores = bell_draw(key_list[11], (TOKENS, TOP), 1.5, 8.0, ((0, 32),), jnp.float32)
    gate_experts = bell_draw(key_list[12], (EXPERTS, D, FF), D ** -0.5, 0.125, ((0, 8),))
    up_experts = bell_draw(key_list[13], (EXPERTS, D, FF), D ** -0.5, 0.125, ((0, 8),))
    down_experts = bell_draw(key_list[14], (EXPERTS, FF, D), FF ** -0.5, 0.25, ((0, 8),))
    return {"conv_outer": conv_outer, "conv_inner": conv_inner, "conv_input": conv_input, "conv_taps": conv_taps, "out_weight": out_weight, "mix_gate": mix_gate, "residual": residual, "mix_gain": mix_gain, "expert_gain": expert_gain, "expert_ids": expert_ids, "group_share": group_share, "pair_scores": pair_scores, "gate_experts": gate_experts, "up_experts": up_experts, "down_experts": down_experts}


epsilon = 1e-06

def rms_scale(values, gain):
    return values * lax.rsqrt(lax.optimization_barrier(jnp.mean(values * values, axis=-1, keepdims=True)) + epsilon) * gain

def reference(conv_outer, conv_inner, conv_input, conv_taps, out_weight, mix_gate, residual, mix_gain, expert_gain, expert_ids, group_share, pair_scores, gate_experts, up_experts, down_experts):
    inner = conv_inner.astype(jnp.float32) * conv_input.astype(jnp.float32)
    length = inner.shape[0]
    padded = jnp.pad(inner, ((KSIZE - 1, 0), (0, 0)))
    conv = conv_taps[0] * padded[0:length]
    for offset in range(1, KSIZE):
        conv = conv + conv_taps[offset] * padded[offset:offset + length]
    mixed_rows = (conv_outer.astype(jnp.float32) * conv).astype(jnp.bfloat16)
    projected = jnp.dot(mixed_rows, out_weight, preferred_element_type=jnp.float32)
    mixed = jax.nn.sigmoid(mix_gate.astype(jnp.float32)) * projected
    hidden_state = (residual.astype(jnp.float32) + rms_scale(mixed, mix_gain)).astype(jnp.bfloat16)
    normed = rms_scale(hidden_state.astype(jnp.float32), expert_gain).astype(jnp.bfloat16)
    flat_ids = expert_ids.reshape(-1).astype(jnp.int32)
    total = flat_ids.shape[0]
    bound = TOKENS // TOK_DEV * CAP

    def one_expert(carried, expert):
        chosen = jnp.nonzero(flat_ids == expert, size=bound, fill_value=total)[0].astype(jnp.int32)
        rows = normed[jnp.minimum(chosen, total - 1) // TOP]
        first = jnp.dot(rows, gate_experts[expert], preferred_element_type=jnp.float32)
        second = jnp.dot(rows, up_experts[expert], preferred_element_type=jnp.float32)
        inner_hidden = (jax.nn.silu(first) * second).astype(jnp.bfloat16)
        result = jnp.dot(inner_hidden, down_experts[expert], preferred_element_type=jnp.float32).astype(jnp.bfloat16)
        return (carried.at[chosen].set(result, mode='drop'), None)
    start = jnp.zeros((total, D), jnp.bfloat16)
    assigned, unused = lax.scan(one_expert, start, jnp.arange(EXPERTS, dtype=jnp.int32))
    assigned = assigned.reshape(TOKENS, TOP, D)
    weights = group_share[:, None] * jax.nn.softmax(pair_scores, axis=-1)
    result = hidden_state.astype(jnp.float32)
    for slot in range(TOP):
        result = result + weights[:, slot:slot + 1] * assigned[:, slot].astype(jnp.float32)
    return result.astype(jnp.bfloat16)
```

```python
import jax
import jax.numpy as jnp
from jax import lax
from jax.sharding import PartitionSpec as P

epsilon = 1e-06


def f32(value):
    return value.astype(jnp.float32)


def bf16(value):
    return value.astype(jnp.bfloat16)


def rms_scale(values, gain):
    return values * lax.rsqrt(jnp.mean(values * values, axis=-1, keepdims=True) + epsilon) * gain


def shifted(value, steps, senders):
    return lax.ppermute(value, "sp", [(s, s + steps) for s in senders])


def swapped(value, axis, bit):
    return lax.ppermute(value, axis, [(s, s ^ bit) for s in range(lax.axis_size(axis))])


def mixer_rows(conv_outer, conv_inner, conv_input, conv_taps):
    kept = conv_taps.shape[0] - 1
    inner = f32(conv_inner) * f32(conv_input)
    tail = f32(conv_inner[-kept:]) * f32(conv_input[-kept:])
    earlier = shifted(tail, 1, range(lax.axis_size("sp") - 1))
    length = conv_inner.shape[0]
    inner = jnp.concatenate([earlier, inner], 0)
    conv = conv_taps[0] * inner[0:length]
    for offset in range(1, kept + 1):
        conv = conv + conv_taps[offset] * inner[offset : offset + length]
    return bf16(f32(conv_outer) * conv)


def project(mixed_rows, out_weight, own_rows):
    parts = lax.axis_size("tp")
    me = lax.axis_index("tp")
    blocks = mixed_rows.reshape(parts, own_rows, -1)

    def partial(owner):
        rows = lax.dynamic_index_in_dim(blocks, owner, 0, keepdims=False)
        return jnp.dot(rows, out_weight, preferred_element_type=jnp.float32)

    def total(owner_bits, bit):
        if bit == 1:
            return partial(me ^ owner_bits)
        half = bit // 2
        given = swapped(bf16(total(owner_bits | half, half)), "tp", half)
        return total(owner_bits, half) + f32(given)

    return total(0, parts)


def per_device(
    conv_outer,
    conv_inner,
    conv_input,
    conv_taps,
    out_weight,
    mix_gate,
    residual,
    mix_gain,
    expert_gain,
    expert_ids,
    group_share,
    pair_scores,
    gate_experts,
    up_experts,
    down_experts,
):
    count = lax.axis_size("sp")
    me = lax.axis_index("sp")
    own_rows = residual.shape[0]
    groups = count // 2
    place = me // 2
    side = lax.axis_index("tp") % 2
    half = gate_experts.shape[2] // 2

    def fetched(weight, axis):
        piece = lax.dynamic_slice_in_dim(weight[0], side * half, half, axis)
        first = swapped(piece, "sp", 1)
        return jnp.concatenate([weight[0], first, swapped(first, "tp", 1)], axis)

    gate_both = fetched(gate_experts, 1)
    up_both = fetched(up_experts, 1)
    down_both = fetched(down_experts, 0)

    weights = group_share[:, None] * jax.nn.softmax(pair_scores, axis=-1)
    experts = jnp.arange(count, dtype=jnp.int32)[:, None]
    table = jnp.zeros((count, own_rows), jnp.float32)
    for slot in range(expert_ids.shape[1]):
        table = table + jnp.where(
            expert_ids[:, slot][None, :] == experts, weights[:, slot][None, :], 0.0
        )

    def spread(own):
        below, above = {0: own}, {0: own}
        for step in range(1, groups):
            below[step] = shifted(below[step - 1], 2, range(2 * (step - 1), count - 2))
            above[step] = shifted(above[step - 1], -2, range(2, count - 2 * (step - 1)))
        order = [(own, None)]
        for near in range(1, (groups - 1) // 2 + 1):
            far = groups - near
            order.append((jnp.where(place < near, above[near], below[near]), near))
            late = jnp.where(place < groups - near, above[near], below[far])
            order.append((jnp.where(place < near, above[far], late), far))
        if groups % 2 == 0:
            mid = groups // 2
            order.append((jnp.where(place < mid, above[mid], below[mid]), mid))
        return sorted(order, key=lambda item: item[1] or 0)

    tables = spread(table)

    mixed_rows = mixer_rows(conv_outer, conv_inner, conv_input, conv_taps)
    projected = project(mixed_rows, out_weight, own_rows)
    mixed = jax.nn.sigmoid(f32(mix_gate)) * projected
    hidden_state = bf16(f32(residual) + rms_scale(mixed, mix_gain))
    normed = bf16(rms_scale(f32(hidden_state), expert_gain))

    blocks = spread(normed)

    def served(rows, shares):
        mine = lax.dynamic_index_in_dim(shares, me, 0, keepdims=False)[:, None]
        other = lax.dynamic_index_in_dim(shares, me ^ 1, 0, keepdims=False)[:, None]
        wide = 2 * half
        first = jnp.dot(rows, gate_both, preferred_element_type=jnp.float32)
        second = jnp.dot(rows, up_both, preferred_element_type=jnp.float32)
        share = jnp.where(jnp.arange(2 * wide)[None, :] < wide, mine, other)
        return jnp.dot(
            bf16(jax.nn.silu(first) * second * share),
            down_both,
            preferred_element_type=jnp.float32,
        )

    results = {
        number or 0: served(rows, shares)
        for (rows, number), (shares, _) in zip(blocks, tables)
    }
    slots = {}
    for near in range(1, (groups - 1) // 2 + 1):
        far = groups - near
        slots[near] = jnp.where(place < near, results[far], results[near])
        slots[far] = jnp.where(place < near, results[near], results[far])
    if groups % 2 == 0:
        slots[groups // 2] = results[groups // 2]

    down = up = None
    for step in range(1, groups):
        gone = groups - step
        lower, upper = slots[gone], slots[step]
        if down is not None:
            lower, upper = lower + f32(down), upper + f32(up)
        down = shifted(bf16(lower), -2, range(2 * gone, count))
        up = shifted(bf16(upper), 2, range(0, count - 2 * gone))
    result = f32(hidden_state) + results[0]
    if down is not None:
        result = result + f32(down) + f32(up)
    return bf16(result)


def solution(mesh):
    placed = (
        P("sp", "tp"),
        P("sp", "tp"),
        P("sp", "tp"),
        P(None, "tp"),
        P("tp", None),
        P(("sp", "tp"), None),
        P(("sp", "tp"), None),
        P(),
        P(),
        P(("sp", "tp"), None),
        P(("sp", "tp")),
        P(("sp", "tp"), None),
        P("sp", None, None),
        P("sp", None, None),
        P("sp", None, None),
    )
    return jax.shard_map(
        per_device, mesh=mesh, in_specs=placed, out_specs=P(("sp", "tp"), None), check_vma=False
    )
```

```python
import jax
import jax.numpy as jnp
from jax import lax
from jax.sharding import PartitionSpec as P

epsilon = 1e-06


def f32(value):
    return value.astype(jnp.float32)


def bf16(value):
    return value.astype(jnp.bfloat16)


def rms_scale(values, gain):
    return values * lax.rsqrt(jnp.mean(values * values, axis=-1, keepdims=True) + epsilon) * gain


def shifted(value, steps, senders):
    return lax.ppermute(value, "sp", [(s, s + steps) for s in senders])


def swapped(value, axis, bit):
    return lax.ppermute(value, axis, [(s, s ^ bit) for s in range(lax.axis_size(axis))])


def mixer_rows(conv_outer, conv_inner, conv_input, conv_taps):
    kept = conv_taps.shape[0] - 1
    inner = f32(conv_inner) * f32(conv_input)
    tail = f32(conv_inner[-kept:]) * f32(conv_input[-kept:])
    earlier = shifted(tail, 1, range(lax.axis_size("sp") - 1))
    length = conv_inner.shape[0]
    inner = jnp.concatenate([earlier, inner], 0)
    conv = conv_taps[0] * inner[0:length]
    for offset in range(1, kept + 1):
        conv = conv + conv_taps[offset] * inner[offset : offset + length]
    return bf16(f32(conv_outer) * conv)


def project(mixed_rows, out_weight, own_rows):
    parts = lax.axis_size("tp")
    me = lax.axis_index("tp")
    blocks = mixed_rows.reshape(parts, own_rows, -1)

    def partial(owner):
        rows = lax.dynamic_index_in_dim(blocks, owner, 0, keepdims=False)
        return jnp.dot(rows, out_weight, preferred_element_type=jnp.float32)

    def total(owner_bits, bit):
        if bit == 1:
            return partial(me ^ owner_bits)
        half = bit // 2
        given = swapped(bf16(total(owner_bits | half, half)), "tp", half)
        return total(owner_bits, half) + f32(given)

    return total(0, parts)


def per_device(
    conv_outer,
    conv_inner,
    conv_input,
    conv_taps,
    out_weight,
    mix_gate,
    residual,
    mix_gain,
    expert_gain,
    expert_ids,
    group_share,
    pair_scores,
    gate_experts,
    up_experts,
    down_experts,
):
    count = lax.axis_size("sp")
    me = lax.axis_index("sp")
    own_rows = residual.shape[0]
    groups = count // 2
    place = me // 2
    side = lax.axis_index("tp") % 2
    half = gate_experts.shape[2] // 2

    def fetched(weight, axis):
        piece = lax.dynamic_slice_in_dim(weight[0], side * half, half, axis)
        first = swapped(piece, "sp", 1)
        second = swapped(first, "tp", 1)
        return jnp.concatenate([weight[0], first, second], axis)

    gate_both = fetched(gate_experts, 1)
    up_both = fetched(up_experts, 1)
    down_both = fetched(down_experts, 0)

    weights = group_share[:, None] * jax.nn.softmax(pair_scores, axis=-1)
    lanes = -(-2 * count // 128) * 128
    column = jnp.arange(lanes, dtype=jnp.int32)[None, :]
    coarse = lax.reduce_precision(weights, 8, 7)
    fine = weights - coarse
    table = jnp.zeros((own_rows, lanes), jnp.float32)
    for slot in range(expert_ids.shape[1]):
        at = expert_ids[:, slot : slot + 1]
        table = table + jnp.where(column == at, coarse[:, slot : slot + 1], 0.0)
        table = table + jnp.where(column == at + count, fine[:, slot : slot + 1], 0.0)
    table = bf16(table)

    def spread(own):
        below, above = {0: own}, {0: own}
        for step in range(1, groups):
            below[step] = shifted(below[step - 1], 2, range(2 * (step - 1), count - 2))
            above[step] = shifted(above[step - 1], -2, range(2, count - 2 * (step - 1)))
        order = {0: own}
        for near in range(1, (groups - 1) // 2 + 1):
            far = groups - near
            early = jnp.where(place < near, above[near], below[near])
            _, over, under, away = lax.optimization_barrier(
                (early, above[near], below[far], above[far])
            )
            order[near] = early
            late = jnp.where(place < far, over, under)
            order[far] = jnp.where(place < near, away, late)
        if groups % 2 == 0:
            mid = groups // 2
            order[mid] = jnp.where(place < mid, above[mid], below[mid])
        return order

    mixed_rows = mixer_rows(conv_outer, conv_inner, conv_input, conv_taps)
    projected = project(mixed_rows, out_weight, own_rows)
    mixed = jax.nn.sigmoid(f32(mix_gate)) * projected
    hidden_state = bf16(f32(residual) + rms_scale(mixed, mix_gain))
    normed = bf16(rms_scale(f32(hidden_state), expert_gain))

    blocks = spread(jnp.concatenate([normed, table], 1))
    depth = normed.shape[1]

    def served(block):
        rows, shares = block[:, :depth], f32(block[:, depth:])

        def share_of(expert):
            chosen = (column == expert) | (column == expert + count)
            return jnp.sum(jnp.where(chosen, shares, 0.0), axis=1, keepdims=True)

        wide = 2 * half
        first = jnp.dot(rows, gate_both, preferred_element_type=jnp.float32)
        second = jnp.dot(rows, up_both, preferred_element_type=jnp.float32)
        mine = jnp.arange(2 * wide)[None, :] < wide
        share = jnp.where(mine, share_of(me), share_of(me ^ 1))
        hidden = lax.optimization_barrier(bf16(jax.nn.silu(first) * second * share))
        return lax.optimization_barrier(
            jnp.dot(hidden, down_both, preferred_element_type=jnp.float32)
        )

    results = {number: served(block) for number, block in blocks.items()}

    def for_upper(step):
        gone = groups - step
        if step == gone or step < gone:
            return results[gone]
        return jnp.where(place < gone, results[gone], results[step])

    down = up = None
    for step in range(1, groups):
        gone = groups - step
        lower, upper = results[gone], for_upper(step)
        if down is not None:
            lower, upper = lower + f32(down), upper + f32(up)
        down = shifted(bf16(lower), -2, range(2 * gone, count))
        up = shifted(bf16(upper), 2, range(0, count - 2 * gone))
    result = f32(hidden_state) + results[0]
    if down is not None:
        result = result + f32(down) + f32(up)
    return bf16(result)


def solution(mesh):
    placed = (
        P("sp", "tp"),
        P("sp", "tp"),
        P("sp", "tp"),
        P(None, "tp"),
        P("tp", None),
        P(("sp", "tp"), None),
        P(("sp", "tp"), None),
        P(),
        P(),
        P(("sp", "tp"), None),
        P(("sp", "tp")),
        P(("sp", "tp"), None),
        P("sp", None, None),
        P("sp", None, None),
        P("sp", None, None),
    )

    return jax.shard_map(
        per_device, mesh=mesh, in_specs=placed, out_specs=P(("sp", "tp"), None), check_vma=False
    )
```

```python
import jax
import jax.numpy as jnp
from jax import lax
from jax.sharding import PartitionSpec as P

epsilon = 1e-06


def f32(value):
    return value.astype(jnp.float32)


def bf16(value):
    return value.astype(jnp.bfloat16)


def rms_scale(values, gain):
    return values * lax.rsqrt(jnp.mean(values * values, axis=-1, keepdims=True) + epsilon) * gain


def shifted(value, steps, senders):
    return lax.ppermute(value, "sp", [(s, s + steps) for s in senders])


def swapped(value, axis, bit):
    return lax.ppermute(value, axis, [(s, s ^ bit) for s in range(lax.axis_size(axis))])


def mixer_rows(conv_outer, conv_inner, conv_input, conv_taps):
    kept = conv_taps.shape[0] - 1
    inner = f32(conv_inner) * f32(conv_input)
    tail = f32(conv_inner[-kept:]) * f32(conv_input[-kept:])
    earlier = shifted(tail, 1, range(lax.axis_size("sp") - 1))
    length = conv_inner.shape[0]
    inner = jnp.concatenate([earlier, inner], 0)
    conv = conv_taps[0] * inner[0:length]
    for offset in range(1, kept + 1):
        conv = conv + conv_taps[offset] * inner[offset : offset + length]
    return bf16(f32(conv_outer) * conv)


def project(mixed_rows, out_weight, own_rows):
    parts = lax.axis_size("tp")
    me = lax.axis_index("tp")
    blocks = mixed_rows.reshape(parts, own_rows, -1)

    def partial(owner):
        rows = lax.dynamic_index_in_dim(blocks, owner, 0, keepdims=False)
        return jnp.dot(rows, out_weight, preferred_element_type=jnp.float32)

    def total(owner_bits, bit):
        if bit == 1:
            return partial(me ^ owner_bits)
        half = bit // 2
        sent = bf16(total(owner_bits | half, half))
        given = swapped(sent, "tp", half)
        return total(owner_bits, half) + f32(given)

    return total(0, parts)


def per_device(
    conv_outer,
    conv_inner,
    conv_input,
    conv_taps,
    out_weight,
    mix_gate,
    residual,
    mix_gain,
    expert_gain,
    expert_ids,
    group_share,
    pair_scores,
    gate_experts,
    up_experts,
    down_experts,
):
    count = lax.axis_size("sp")
    me = lax.axis_index("sp")
    own_rows = residual.shape[0]
    groups = count // 2
    place = me // 2
    side = lax.axis_index("tp") % 2
    half = gate_experts.shape[2] // 2

    def fetched(weight, axis):
        piece = lax.dynamic_slice_in_dim(weight[0], side * half, half, axis)
        first = swapped(piece, "sp", 1)
        second = swapped(first, "tp", 1)
        return jnp.concatenate([weight[0], first, second], axis)

    gate_both = fetched(gate_experts, 1)
    up_both = fetched(up_experts, 1)
    down_both = fetched(down_experts, 0)

    weights = group_share[:, None] * jax.nn.softmax(pair_scores, axis=-1)
    lanes = -(-2 * count // 128) * 128
    column = jnp.arange(lanes, dtype=jnp.int32)[None, :]
    coarse = lax.reduce_precision(weights, 8, 7)
    fine = weights - coarse
    table = jnp.zeros((own_rows, lanes), jnp.float32)
    for slot in range(expert_ids.shape[1]):
        at = expert_ids[:, slot : slot + 1]
        table = table + jnp.where(column == at, coarse[:, slot : slot + 1], 0.0)
        table = table + jnp.where(column == at + count, fine[:, slot : slot + 1], 0.0)
    table = bf16(table)

    def spread(own):
        below, above = {0: own}, {0: own}
        for step in range(1, groups):
            below[step] = shifted(below[step - 1], 2, range(2 * (step - 1), count - 2))
            above[step] = shifted(above[step - 1], -2, range(2, count - 2 * (step - 1)))
        order = {0: own}
        for near in range(1, (groups - 1) // 2 + 1):
            far = groups - near
            early = jnp.where(place < near, above[near], below[near])
            _, over, under, away = lax.optimization_barrier(
                (early, above[near], below[far], above[far])
            )
            order[near] = early
            late = jnp.where(place < far, over, under)
            order[far] = jnp.where(place < near, away, late)
        if groups % 2 == 0:
            mid = groups // 2
            order[mid] = jnp.where(place < mid, above[mid], below[mid])
        return order

    mixed_rows = mixer_rows(conv_outer, conv_inner, conv_input, conv_taps)
    projected = project(mixed_rows, out_weight, own_rows)
    mixed = jax.nn.sigmoid(f32(mix_gate)) * projected
    hidden_state = bf16(f32(residual) + rms_scale(mixed, mix_gain))
    normed = bf16(rms_scale(f32(hidden_state), expert_gain))

    blocks = spread(jnp.concatenate([normed, table], 1))
    depth = normed.shape[1]

    def served(block):
        rows = block[:, :depth]
        chosen = jnp.arange(lanes, dtype=jnp.int32)[:, None] % count
        picks = bf16(chosen == jnp.stack([me, me ^ 1])[None, :])
        picks = jnp.where(jnp.arange(lanes)[:, None] < 2 * count, picks, 0)
        shares = jnp.dot(block[:, depth:], picks, preferred_element_type=jnp.float32)
        wide = 2 * half
        first = jnp.dot(rows, gate_both, preferred_element_type=jnp.float32)
        second = jnp.dot(rows, up_both, preferred_element_type=jnp.float32)
        mine = jnp.arange(2 * wide)[None, :] < wide
        share = jnp.where(mine, shares[:, :1], shares[:, 1:])
        hidden = lax.optimization_barrier(bf16(jax.nn.silu(first) * second * share))
        return lax.optimization_barrier(
            jnp.dot(hidden, down_both, preferred_element_type=jnp.float32)
        )

    results = {number: served(block) for number, block in blocks.items()}

    def for_upper(step):
        gone = groups - step
        if step == gone or step < gone:
            return results[gone]
        return jnp.where(place < gone, results[gone], results[step])

    down = up = None
    for step in range(1, groups):
        gone = groups - step
        lower, upper = results[gone], for_upper(step)
        if down is not None:
            lower, upper = lower + f32(down), upper + f32(up)
        down = shifted(bf16(lower), -2, range(2 * gone, count))
        up = shifted(bf16(upper), 2, range(0, count - 2 * gone))
    result = f32(hidden_state) + results[0]
    if down is not None:
        result = result + f32(down) + f32(up)
    return bf16(result)


def solution(mesh):
    placed = (
        P("sp", "tp"),
        P("sp", "tp"),
        P("sp", "tp"),
        P(None, "tp"),
        P("tp", None),
        P(("sp", "tp"), None),
        P(("sp", "tp"), None),
        P(),
        P(),
        P(("sp", "tp"), None),
        P(("sp", "tp")),
        P(("sp", "tp"), None),
        P("sp", None, None),
        P("sp", None, None),
        P("sp", None, None),
    )

    return jax.shard_map(
        per_device, mesh=mesh, in_specs=placed, out_specs=P(("sp", "tp"), None), check_vma=False
    )
```
